32 devices in a mesh: ep: 8 (over z, x), tp: 4 (over y, core).
Axes of the slice: x: 2, y: 2, z: 4, core: 2. Of those that a mesh axis runs over, the one named last changes fastest.
Arguments:
- tokens_a: bfloat16 [1024, 2048], P('ep'), may hold values from -6 to 6
- gain_a: float32 [2048], replicated, may hold values from 0.1 to 1.9
- value_w: bfloat16 [2048, 2048], P(None, 'tp'), may hold values from -0.125 to 0.125
- gate_w: bfloat16 [2048, 2048], P(None, 'tp'), may hold values from -0.125 to 0.125
- kernel: float32 [31, 2048], P(None, 'tp')
- chan_gain: float32 [2048], P('tp'), may hold values from 0.1 to 1.9
- out_w: bfloat16 [2048, 2048], P('tp'), may hold values from -0.125 to 0.125
- tokens_b: bfloat16 [1536, 2048], P('ep'), may hold values from -6 to 6
- gain_b: float32 [2048], replicated, may hold values from 0.1 to 1.9
- routes: int32 [1536, 2], P('ep'), may hold values from 0 to 7, all different within a row; in each aligned block of 192 rows (0 to 191, 192 to 383, ...) at most 72 rows name the same one
- route_logits: float32 [1536, 2], P('ep'), may hold values from -6 to 6
- expert_gate: bfloat16 [8, 2048, 2816], P('ep', None, 'tp'), may hold values from -0.125 to 0.125
- expert_up: bfloat16 [8, 2048, 2816], P('ep', None, 'tp'), may hold values from -0.125 to 0.125
- expert_down: bfloat16 [8, 2816, 2048], P('ep', 'tp'), may hold values from -0.109375 to 0.109375
Outputs:
- conv_out: bfloat16 [2048, 1024], P('tp', 'ep')
- moe_out: bfloat16 [2048, 1536], P('tp', 'ep')
The draws below stay inside these ranges and needn't reach their ends.
Inputs may be any that keep to these rules, and one draw needn't show every extreme that they name: `routes`: each row names 2 different experts; among the rows of one index of ep no expert is named by more than 72 rows, a bound that some block reaches.
All inputs are finite; a program needn't handle non-finite values.
Results may differ from the reference program's by a relative error of at most 0.018.
Values may be sent and summed in bfloat16 or wider, within the bound.
No kernel may reach another device: no remote copies, remote signals or barrier semaphores. Data moves between devices by JAX's collectives and lax.ppermute only.
A program may use at most 64 MiB of HBM per device.

```python
import math
import jax
import jax.numpy as jnp
import numpy as np
from jax import lax

D = 2048
CONV_CH = 2048
KWIDTH = 31
FF = 2816
TOPK = 2
ROWS_B = 192
EXPERTS = 8
CAP = 72
TOKENS_A = 1024
TOKENS_B = 1536
N_EP = 8
N_TP = 4


def draw_kernel(key, part):
    first, second = jax.random.split(key)
    ramp = 1.0 + 3.0 * jnp.arange(CONV_CH, dtype=jnp.float32) / CONV_CH
    base = jax.random.normal(first, (KWIDTH, CONV_CH), jnp.float32)
    rough = jax.random.uniform(second, (1, CONV_CH), jnp.float32, 0.5, 1.5)
    return base * rough * ramp[None, :] / math.sqrt(KWIDTH)


def block_scale(rng, dims, pieces, smallest, high):
    def one(position, parts):
        heights = jax.random.uniform(jax.random.fold_in(jax.random.fold_in(rng, 6), position), (parts,), jnp.float32, smallest / len(pieces), high / len(pieces))
        return jnp.repeat(jnp.exp(heights), dims[position] // parts).reshape((-1,) + (1,) * (len(dims) - position - 1))

    loudness = one(*pieces[0])
    for cut in pieces[1:]:
        loudness = loudness * one(*cut)
    return loudness


def deal_out(rng, own, number, rows, amount, top, most, slope):
    order = jax.random.permutation(rng, amount)
    heavy_load, ordinary = load_shares(amount, rows * top, most, slope, True), load_shares(amount, rows * top, most, slope, False)
    places = jnp.arange(amount)

    def named(tallies, offset_by):
        used = int((tallies > 0).sum())
        fixed = max(1, used // 4)
        passed = fixed + (places - fixed + offset_by * (used - fixed)) % max(1, amount - fixed)
        return jnp.zeros((amount,), jnp.int32).at[order[jnp.where(places < fixed, places, passed)]].set(jnp.asarray(tallies, jnp.int32))

    tallies = jnp.where(number % 4 == 0, named(heavy_load, number // 4), named(ordinary, number - number // 4 - 1))
    mixed = jax.random.permutation(jax.random.fold_in(own, 3), amount)
    source_of, taker = mixed[0:amount // 2 * 2:2], mixed[1:amount // 2 * 2:2]
    room = jnp.minimum(tallies[source_of] - 1, most - tallies[taker]) // 2
    room = jnp.where((source_of == order[0]) | (taker == order[0]) | (tallies[taker] == 0), 0, jnp.maximum(room, 0))
    passed = jax.random.randint(jax.random.fold_in(own, 4), (amount // 2,), 0, 1 << 20) % (room + 1)
    tallies = tallies.at[source_of].add(-passed).at[taker].add(passed)
    members = jnp.searchsorted(jnp.cumsum(tallies), jnp.arange(rows * top), side="right").astype(jnp.int32)
    listing = members.reshape(top, rows).T
    listing = listing[jax.random.permutation(jax.random.fold_in(own, 1), rows)]
    offset_by = jax.random.randint(jax.random.fold_in(own, 2), (rows, 1), 0, top)
    return jnp.take_along_axis(listing, (jnp.arange(top)[None, :] + offset_by) % top, axis=1)


def load_shares(count, total, bound, slope, full):
    weights = [(1 << 20) // math.isqrt(grade ** slope) + 1 for grade in range(1, count + 1)]
    largest = bound if full else min(bound, max(-(-total // count), total * weights[0] // sum(weights)))
    least = 1 if total - largest >= count - 1 else 0
    counts, spare = [largest] + [least] * (count - 1), total - largest - least * (count - 1)
    while spare > 0:
        free = [i for i in range(1, count) if counts[i] < largest] or [i for i in range(1, count) if counts[i] < bound]
        pool, budget = sum([weights[i] for i in free]), spare
        for i in free:
            more = min(bound - counts[i], max(1, budget * weights[i] // pool), spare)
            counts[i] = counts[i] + more
            spare = spare - more
    return np.array(counts)


def gaussian(own_key, dims, scale, limit, cuts=(), held_as=jnp.bfloat16):
    array = scale * jax.random.normal(own_key, dims, jnp.float32)
    if cuts:
        array = array * block_scale(own_key, dims, cuts, -0.22, 0.18)
    return jnp.clip(array, -limit, limit).astype(held_as)


def setup_inputs(seed: int = 0) -> dict:
    arg_keys = jax.random.split(jax.random.key(seed), 15)
    tokens_a = gaussian(arg_keys[0], (TOKENS_A, D), 1.0, 6.0, ((0, 8),))
    gain_a = jnp.clip(1.0 + 0.18 * jax.random.normal(arg_keys[1], (D,), jnp.float32), 0.1, 1.9)
    value_w = gaussian(arg_keys[2], (D, CONV_CH), D ** -0.5, 0.125, ((1, 4),))
    gate_w = gaussian(arg_keys[3], (D, CONV_CH), D ** -0.5, 0.125, ((1, 4),))
    kernel = draw_kernel(jax.random.fold_in(arg_keys[14], 71), 0)
    chan_gain = jnp.clip(1.0 + 0.18 * jax.random.normal(arg_keys[5], (CONV_CH,), jnp.float32), 0.1, 1.9)
    out_w = gaussian(arg_keys[6], (CONV_CH, D), CONV_CH ** -0.5, 0.125, ((0, 4),))
    tokens_b = gaussian(arg_keys[7], (TOKENS_B, D), 1.0, 6.0, ((0, 8),))
    gain_b = jnp.clip(1.0 + 0.18 * jax.random.normal(arg_keys[8], (D,), jnp.float32), 0.1, 1.9)
    routes_keys = jax.random.split(jax.random.fold_in(arg_keys[9], 1), TOKENS_B // ROWS_B)
    routes_turns = jax.random.permutation(jax.random.fold_in(arg_keys[9], 3), TOKENS_B // ROWS_B)
    routes = jax.vmap(lambda own, number: deal_out(jax.random.fold_in(arg_keys[9], 2), own, number, ROWS_B, EXPERTS, TOPK, CAP, 1))(routes_keys, routes_turns).reshape((TOKENS_B, TOPK))
    route_logits = gaussian(arg_keys[10], (TOKENS_B, TOPK), 1.0, 6.0, ((0, 8),), jnp.float32)
    expert_gate = gaussian(arg_keys[11], (EXPERTS, D, FF), D ** -0.5, 0.125, ((0, 8), (2, 4)))
    expert_up = gaussian(arg_keys[12], (EXPERTS, D, FF), D ** -0.5, 0.125, ((0, 8), (2, 4)))
    expert_down = gaussian(arg_keys[13], (EXPERTS, FF, D), FF ** -0.5, 0.109375, ((0, 8), (1, 4)))
    return dict(tokens_a=tokens_a, gain_a=gain_a, value_w=value_w, gate_w=gate_w, kernel=kernel, chan_gain=chan_gain, out_w=out_w, tokens_b=tokens_b, gain_b=gain_b, routes=routes, route_logits=route_logits, expert_gate=expert_gate, expert_up=expert_up, expert_down=expert_down)


def rms_scaled(tokens, gain):
    values = tokens.astype(jnp.float32)
    scaled = values * lax.rsqrt(lax.optimization_barrier(jnp.mean(values * values, axis=1, keepdims=True)) + 1e-06)
    return (scaled * gain[None, :]).astype(jnp.bfloat16)

def slot_table(route_rows, experts, capacity):
    flat_expert = route_rows.reshape(-1).astype(jnp.int32)
    expert_ids = jnp.arange(experts, dtype=jnp.int32)
    onehot = (flat_expert[:, None] == expert_ids[None, :]).astype(jnp.int32)
    before = jnp.cumsum(onehot, axis=0).astype(jnp.int32) - onehot
    ranking = lax.optimization_barrier(jnp.sum(before * onehot, axis=1)).astype(jnp.int32)
    return (flat_expert * capacity + ranking).astype(jnp.int32)

def reference(tokens_a, gain_a, value_w, gate_w, kernel, chan_gain, out_w, tokens_b, gain_b, routes, route_logits, expert_gate, expert_up, expert_down):
    normed = rms_scaled(tokens_a, gain_a)
    value_part = jnp.dot(normed, value_w, preferred_element_type=jnp.float32)
    gate_part = jnp.dot(normed, gate_w, preferred_element_type=jnp.float32)
    glu = (value_part * jax.nn.sigmoid(gate_part)).astype(jnp.bfloat16)
    glu = lax.optimization_barrier(glu).astype(jnp.float32)
    length = glu.shape[0]
    padded = jnp.concatenate([jnp.zeros((KWIDTH - 1, CONV_CH), jnp.float32), glu], axis=0)
    mixed = jnp.zeros((length, CONV_CH), jnp.float32)
    for tap in range(KWIDTH):
        mixed = mixed + kernel[tap][None, :] * padded[tap:tap + length]
    average = lax.optimization_barrier(jnp.mean(mixed, axis=1, keepdims=True))
    spread = lax.optimization_barrier(jnp.mean(mixed * mixed, axis=1, keepdims=True)) - average * average
    activated = jax.nn.silu((mixed - average) * lax.rsqrt(spread + 1e-05) * chan_gain[None, :]).astype(jnp.bfloat16)
    group = CONV_CH // N_TP
    conv_sum = jnp.zeros((length, D), jnp.float32)
    for index in range(N_TP):
        partial_term = jnp.dot(activated[:, index * group:(index + 1) * group], out_w[index * group:(index + 1) * group], preferred_element_type=jnp.float32).astype(jnp.bfloat16)
        conv_sum = conv_sum + lax.optimization_barrier(partial_term).astype(jnp.float32)
    conv_out = conv_sum.astype(jnp.bfloat16).T
    normed_b = rms_scaled(tokens_b, gain_b)
    per_block = TOKENS_B // N_EP
    route_blocks = routes.reshape(N_EP, per_block, TOPK)

    def block_slots(route_rows):
        return slot_table(route_rows, EXPERTS, CAP)
    slot_blocks = jax.vmap(block_slots)(route_blocks)
    block_ids = jnp.arange(N_EP, dtype=jnp.int32)
    owners = (jnp.arange(per_block * TOPK, dtype=jnp.int32) // TOPK)[None, :] + block_ids[:, None] * per_block

    def block_fill(slots, owner_rows):
        return jnp.zeros((EXPERTS * CAP,), jnp.int32).at[slots].set(owner_rows + 1)
    filled = jax.vmap(block_fill)(slot_blocks, owners)
    index_table = jnp.transpose(filled.reshape(N_EP, EXPERTS, CAP), (1, 0, 2)).reshape(EXPERTS, N_EP * CAP) - 1
    group_ff = FF // N_TP

    def expert_apply(operands):
        index_rows, gate_e, up_e, down_e = operands
        picked = jnp.take(normed_b, jnp.maximum(index_rows, 0), axis=0)
        picked = jnp.where((index_rows >= 0)[:, None], picked, jnp.zeros_like(picked))
        gate_act = jnp.dot(picked, gate_e, preferred_element_type=jnp.float32)
        up_act = jnp.dot(picked, up_e, preferred_element_type=jnp.float32)
        hidden = (jax.nn.silu(gate_act) * up_act).astype(jnp.bfloat16)
        hidden_groups = hidden.reshape(-1, N_TP, group_ff).astype(jnp.float32)
        down_groups = down_e.reshape(N_TP, group_ff, D).astype(jnp.float32)
        partial_terms = jnp.einsum('sgf,gfd->gsd', hidden_groups, down_groups).astype(jnp.bfloat16)
        partial_terms = lax.optimization_barrier(partial_terms)
        return lax.optimization_barrier(jnp.sum(partial_terms.astype(jnp.float32), axis=0)).astype(jnp.bfloat16)
    results = lax.map(expert_apply, (index_table, expert_gate, expert_up, expert_down))
    results_flat = results.reshape(EXPERTS * N_EP * CAP, D)
    expert_flat = route_blocks.reshape(N_EP, per_block * TOPK)
    ranking = slot_blocks - expert_flat * CAP
    flat_index = expert_flat * (N_EP * CAP) + block_ids[:, None] * CAP + ranking
    values = jnp.take(results_flat, flat_index.reshape(-1), axis=0).astype(jnp.float32).reshape(TOKENS_B, TOPK, D)
    weights = jax.nn.softmax(route_logits, axis=1)
    moe_out = lax.optimization_barrier(jnp.sum(weights[:, :, None] * values, axis=1)).astype(jnp.bfloat16).T
    return (conv_out, moe_out)
```

```python
import functools

import jax
import jax.numpy as jnp
from jax import lax
from jax.experimental import pallas as pl
from jax.experimental.pallas import tpu as pltpu
from jax.sharding import PartitionSpec as P

F32 = jnp.float32
BF16 = jnp.bfloat16


def swap(block, axis, bit):
    count = lax.axis_size(axis)
    return lax.ppermute(block, axis, [(i, i ^ bit) for i in range(count)])


def tp_bits():
    bits, bit = [], 1
    while bit < lax.axis_size("tp"):
        bits.append(bit)
        bit *= 2
    return bits


def block_order(bits):
    order = [0]
    for bit in reversed(bits):
        order = order + [o ^ bit for o in order]
    return order


def from_behind(block, axis, distance):
    devices = range(lax.axis_size(axis))
    route = [(i - distance, i) for i in devices if i - distance in devices]
    return lax.ppermute(block, axis, route)


def rms_scaled(tokens, gain):
    values = tokens.astype(F32)
    scaled = values * lax.rsqrt(jnp.mean(values * values, axis=1, keepdims=True) + 1e-06)
    return (scaled * gain[None, :]).astype(BF16)


def prep_kernel(tokens, gain, routes, logits, send, comb_hi, comb_lo, *, experts, capacity, block):
    own = lax.axis_index("tp") * block
    me = lax.axis_index("ep")
    rows = tokens.shape[0]
    values = tokens[...].astype(F32)
    scale = lax.rsqrt(jnp.mean(values * values, axis=1, keepdims=True) + 1e-06)
    mine = tokens[:, pl.ds(pl.multiple_of(own, 128), block)].astype(F32)
    normed = (mine * scale * gain[0:1, pl.ds(pl.multiple_of(own, 128), block)]).astype(BF16)
    choices = routes.shape[1]
    ids = lax.broadcasted_iota(jnp.int32, (rows, 128), 1)
    hots = [(routes[:, k : k + 1] == ids).astype(F32) for k in range(choices)]
    total = functools.reduce(lambda a, b: a + b, hots)
    tri = (
        lax.broadcasted_iota(jnp.int32, (rows, rows), 0)
        > lax.broadcasted_iota(jnp.int32, (rows, rows), 1)
    ).astype(BF16)
    before = jnp.dot(tri, total.astype(BF16), preferred_element_type=F32)
    top = jnp.max(logits[...], axis=1, keepdims=True)
    exps = [jnp.exp(logits[:, k : k + 1] - top) for k in range(choices)]
    denom = functools.reduce(lambda a, b: a + b, exps)
    slot_ids = lax.broadcasted_iota(jnp.int32, (rows, experts * capacity), 1)
    placed = jnp.zeros((rows, experts * capacity), F32)
    weighted = jnp.zeros((rows, experts * capacity), F32)
    for k in range(choices):
        rank = jnp.sum(before * hots[k], axis=1, keepdims=True).astype(jnp.int32)
        slot = (routes[:, k : k + 1] ^ me) * capacity + rank
        hit = slot == slot_ids
        placed = placed + jnp.where(hit, 1.0, 0.0)
        weighted = weighted + jnp.where(hit, exps[k] / denom, 0.0)
    high = weighted.astype(BF16)
    comb_hi[...] = high
    comb_lo[...] = (weighted - high.astype(F32)).astype(BF16)
    send[...] = lax.dot_general(
        placed.astype(BF16), normed, (((0,), (0,)), ((), ())), preferred_element_type=F32
    ).astype(BF16)


def ffn_kernel(*refs, order, block, halves):
    xs = refs[:halves]
    gate_h, up_h, down_h, out_send, hidden, gate_v, up_v, down_v, sems = refs[halves:]
    t = lax.axis_index("tp")
    parts = len(order)
    per = parts // halves

    def weight(i):
        row = pl.multiple_of((t ^ order[i]) * block, 128)
        return [
            pltpu.make_async_copy(gate_h.at[pl.ds(row, block)], gate_v.at[i], sems.at[0, i]),
            pltpu.make_async_copy(up_h.at[pl.ds(row, block)], up_v.at[i], sems.at[1, i]),
        ]

    def down(i):
        col = pl.multiple_of((t ^ order[i]) * block, 128)
        return pltpu.make_async_copy(down_h.at[:, pl.ds(col, block)], down_v.at[i - parts // 2], sems.at[2, i])

    for i in range(parts):
        for copy in weight(i):
            copy.start()
    for i in range(parts // 2, parts):
        down(i).start()
    gate = up = None
    for i in range(parts):
        for copy in weight(i):
            copy.wait()
        x = xs[i // per][:, (i % per) * block : (i % per + 1) * block]
        g = jnp.dot(x, gate_v[i], preferred_element_type=F32)
        u = jnp.dot(x, up_v[i], preferred_element_type=F32)
        gate = g if gate is None else gate + g
        up = u if up is None else up + u
    act = (gate * jax.nn.sigmoid(gate) * up).astype(BF16)
    hidden[...] = act
    for i in range(parts // 2, parts):
        down(i).wait()
        j = i - parts // 2
        out_send[:, j * block : (j + 1) * block] = jnp.dot(
            act, down_v[j], preferred_element_type=F32
        ).astype(BF16)


def keep_kernel(hidden, down_h, out_keep, down_v, sems, *, order, block):
    t = lax.axis_index("tp")
    count = len(order) // 2

    def down(i):
        col = pl.multiple_of((t ^ order[i]) * block, 128)
        return pltpu.make_async_copy(down_h.at[:, pl.ds(col, block)], down_v.at[i], sems.at[i])

    for i in range(count):
        down(i).start()
    act = hidden[...]
    for i in range(count):
        down(i).wait()
        out_keep[:, i * block : (i + 1) * block] = jnp.dot(
            act, down_v[i], preferred_element_type=F32
        ).astype(BF16)


def halve(values, bit):
    rows = values.shape[0] // 2
    side = (lax.axis_index("tp") // bit) % 2
    keep = lax.dynamic_slice_in_dim(values, side * rows, rows, 0)
    other = lax.dynamic_slice_in_dim(values, (1 - side) * rows, rows, 0)
    return keep, swap(other, "tp", bit)


def body(
    tokens_a,
    gain_a,
    value_w,
    gate_w,
    kernel,
    chan_gain,
    out_w,
    tokens_b,
    gain_b,
    routes,
    route_logits,
    expert_gate,
    expert_up,
    expert_down,
):
    experts = lax.axis_size("ep")
    bits = tp_bits()
    order = block_order(bits)
    parts = len(order)
    token_count, width = tokens_b.shape
    choices_per = routes.shape[1]
    capacity = 3 * token_count * choices_per // (2 * experts)
    block = width // parts
    slots = experts * capacity
    vmem = pl.BlockSpec(memory_space=pltpu.VMEM)
    anyw = pl.BlockSpec(memory_space=pl.ANY)

    send, comb_hi, comb_lo = pl.pallas_call(
        functools.partial(prep_kernel, experts=experts, capacity=capacity, block=block),
        out_shape=(
            jax.ShapeDtypeStruct((slots, block), BF16),
            jax.ShapeDtypeStruct((token_count, slots), BF16),
            jax.ShapeDtypeStruct((token_count, slots), BF16),
        ),
        in_specs=[vmem] * 4,
        out_specs=(vmem,) * 3,
        name="prep",
    )(tokens_b, gain_b[None, :], routes, route_logits)
    pieces = []
    for d in range(experts):
        piece = send[d * capacity : (d + 1) * capacity]
        piece = swap(piece, "ep", d) if d else piece
        for bit in reversed(bits[1:]):
            piece = jnp.concatenate([piece, swap(piece, "tp", bit)], axis=1)
        pieces.append(piece)
    near = jnp.concatenate(pieces, axis=0)
    inputs = [near, swap(near, "tp", bits[0])]

    normed = rms_scaled(tokens_a, gain_a)
    contract_first = (((0,), (1,)), ((), ()))
    value_part = lax.dot_general(value_w, normed, contract_first, preferred_element_type=F32)
    gate_part = lax.dot_general(gate_w, normed, contract_first, preferred_element_type=F32)
    glu = (value_part * jax.nn.sigmoid(gate_part)).astype(BF16)
    taps = kernel.shape[0]
    length = glu.shape[1]
    rim = from_behind(glu[:, length - (taps - 1) :], "ep", 1)
    padded = jnp.concatenate([rim, glu], axis=1).astype(F32)
    mixed = jnp.zeros(glu.shape, F32)
    for tap in range(taps):
        mixed = mixed + kernel[tap][:, None] * padded[:, tap : tap + length]
    stats = jnp.stack([jnp.sum(mixed, axis=0), jnp.sum(mixed * mixed, axis=0)])
    for bit in bits:
        stats = stats + swap(stats, "tp", bit)
    channels = mixed.shape[0] * parts
    average = stats[0] / channels
    spread = stats[1] / channels - average * average
    normal_out = (
        (mixed - average[None, :]) * lax.rsqrt(spread + 1e-05)[None, :] * chan_gain[:, None]
    )
    activated = jax.nn.silu(normal_out).astype(BF16)
    conv = lax.dot_general(
        out_w, activated, (((0,), (0,)), ((), ())), preferred_element_type=F32
    ).astype(BF16)
    half_blocks = conv.reshape(parts, width // parts, length)
    t = lax.axis_index("tp")
    remaining = list(order)
    picked = [
        lax.dynamic_index_in_dim(half_blocks, t ^ o, 0, keepdims=False) for o in remaining
    ]
    conv_out = jnp.concatenate(picked, axis=0)
    for bit in bits:
        rows = conv_out.shape[0] // 2
        got = swap(conv_out[rows:], "tp", bit)
        conv_out = (conv_out[:rows].astype(F32) + got.astype(F32)).astype(BF16)

    halves = len(inputs)
    ff = expert_gate.shape[2]
    out_send, hidden = pl.pallas_call(
        functools.partial(ffn_kernel, order=order, block=block, halves=halves),
        out_shape=(
            jax.ShapeDtypeStruct((slots, width // 2), BF16),
            jax.ShapeDtypeStruct((slots, ff), BF16),
        ),
        in_specs=[vmem] * halves + [anyw] * 3,
        out_specs=(vmem, vmem),
        scratch_shapes=[
            pltpu.VMEM((parts, block, ff), BF16),
            pltpu.VMEM((parts, block, ff), BF16),
            pltpu.VMEM((parts // 2, ff, block), BF16),
            pltpu.SemaphoreType.DMA((3, parts)),
        ],
        name="ffn",
        cost_estimate=pl.CostEstimate(
            flops=5 * slots * width * ff, bytes_accessed=5 * width * ff, transcendentals=slots * ff
        ),
    )(*inputs, expert_gate[0], expert_up[0], expert_down[0])
    out_keep = pl.pallas_call(
        functools.partial(keep_kernel, order=order, block=block),
        out_shape=jax.ShapeDtypeStruct((slots, width // 2), BF16),
        in_specs=[vmem, anyw],
        out_specs=vmem,
        scratch_shapes=[
            pltpu.VMEM((parts // 2, ff, block), BF16),
            pltpu.SemaphoreType.DMA((parts // 2,)),
        ],
        name="keep",
        cost_estimate=pl.CostEstimate(
            flops=slots * width * ff, bytes_accessed=width * ff, transcendentals=0
        ),
    )(hidden, expert_down[0])
    core_got = swap(out_send, "tp", bits[0])
    returned = [None] * experts
    for d in reversed(range(experts)):
        rows = slice(d * capacity, (d + 1) * capacity)
        piece = (out_keep[rows].astype(F32) + core_got[rows].astype(F32)).astype(BF16)
        for bit in bits[1:]:
            cols = piece.shape[1] // 2
            got = swap(piece[:, cols:], "tp", bit)
            piece = (piece[:, :cols].astype(F32) + got.astype(F32)).astype(BF16)
        returned[d] = swap(piece, "ep", d) if d else piece
    rows = jnp.concatenate(returned, axis=0)
    last = (((0,), (1,)), ((), ()))
    moe_out = lax.dot_general(rows, comb_hi, last, preferred_element_type=F32)
    moe_out = moe_out + lax.dot_general(rows, comb_lo, last, preferred_element_type=F32)
    return (conv_out, moe_out.astype(BF16))


def solution(mesh):
    return jax.shard_map(
        body,
        mesh=mesh,
        in_specs=(
            P("ep", None),
            P(),
            P(None, "tp"),
            P(None, "tp"),
            P(None, "tp"),
            P("tp"),
            P("tp", None),
            P("ep", None),
            P(),
            P("ep", None),
            P("ep", None),
            P("ep", None, "tp"),
            P("ep", None, "tp"),
            P("ep", "tp", None),
        ),
        out_specs=(P("tp", "ep"), P("tp", "ep")),
        check_vma=False,
    )
```

```python
import functools

import jax
import jax.numpy as jnp
from jax import lax
from jax.experimental import pallas as pl
from jax.experimental.pallas import tpu as pltpu
from jax.sharding import PartitionSpec as P


F32 = jnp.float32
BF16 = jnp.bfloat16


def swap(block, axis, bit):
    count = lax.axis_size(axis)
    return lax.ppermute(block, axis, [(i, i ^ bit) for i in range(count)])


def tp_bits():
    bits, bit = [], 1
    while bit < lax.axis_size("tp"):
        bits.append(bit)
        bit *= 2
    return bits


def block_order(bits):
    order = [0]
    for bit in reversed(bits):
        order = order + [o ^ bit for o in order]
    return order


def from_behind(block, axis, distance):
    devices = range(lax.axis_size(axis))
    route = [(i - distance, i) for i in devices if i - distance in devices]
    return lax.ppermute(block, axis, route)


def rms_scaled(tokens, gain):
    values = tokens.astype(F32)
    scaled = values * lax.rsqrt(jnp.mean(values * values, axis=1, keepdims=True) + 1e-06)
    return (scaled * gain[None, :]).astype(BF16)


def prep_kernel(tokens, gain, routes, logits, comb_hi, comb_lo, *send, experts, capacity, block):
    own = lax.axis_index("tp") * block
    me = lax.axis_index("ep")
    rows = tokens.shape[0]
    values = tokens[...].astype(F32)
    scale = lax.rsqrt(jnp.mean(values * values, axis=1, keepdims=True) + 1e-06)
    mine = tokens[:, pl.ds(pl.multiple_of(own, 128), block)].astype(F32)
    normed = (mine * scale * gain[0:1, pl.ds(pl.multiple_of(own, 128), block)]).astype(BF16)
    choices = routes.shape[0]
    ids = lax.broadcasted_iota(jnp.int32, (max(experts, 8), rows), 0)
    hots = [(routes[k : k + 1, :] == ids).astype(F32) for k in range(choices)]
    total = functools.reduce(lambda a, b: a + b, hots)
    tri = (
        lax.broadcasted_iota(jnp.int32, (rows, rows), 0)
        < lax.broadcasted_iota(jnp.int32, (rows, rows), 1)
    ).astype(BF16)
    before = jnp.dot(total.astype(BF16), tri, preferred_element_type=F32)
    top = jnp.max(logits[...], axis=0, keepdims=True)
    exps = [jnp.exp(logits[k : k + 1, :] - top) for k in range(choices)]
    denom = functools.reduce(lambda a, b: a + b, exps)
    slot_ids = lax.broadcasted_iota(jnp.int32, (experts * capacity, rows), 0)
    placed = jnp.zeros((experts * capacity, rows), F32)
    weighted = jnp.zeros((experts * capacity, rows), F32)
    for k in range(choices):
        rank = jnp.sum(before * hots[k], axis=0, keepdims=True).astype(jnp.int32)
        slot = (routes[k : k + 1, :] ^ me) * capacity + rank
        hit = slot == slot_ids
        placed = jnp.where(hit, 1.0, placed)
        weighted = jnp.where(hit, exps[k] / denom, weighted)
    high = weighted.astype(BF16)
    comb_hi[...] = high
    comb_lo[...] = (weighted - high.astype(F32)).astype(BF16)
    sent = jnp.dot(placed.astype(BF16), normed, preferred_element_type=F32).astype(BF16)
    for d in range(experts):
        send[d][...] = sent[d * capacity : (d + 1) * capacity]


def ffn_kernel(*refs, order, block, starts_x):
    parts = len(order)
    n_in = len(starts_x) * parts
    xs = refs[:n_in]
    gate_h, up_h, down_h = refs[n_in : n_in + 3]
    outs = refs[n_in + 3 : n_in + 3 + parts]
    x_v, gate_v, up_v, down_v, hid_v, out_v, xsems, wsems, dsems, osems = refs[n_in + 3 + parts :]
    t = lax.axis_index("tp")
    ff = hid_v.shape[1]
    chunk = 256
    starts = list(range(0, ff, chunk))

    def tokens(g, i):
        ref = xs[g * parts + i]
        to = x_v.at[pl.ds(starts_x[g], ref.shape[0]), pl.ds(i * block, block)]
        return pltpu.make_async_copy(ref, to, xsems.at[g, i])

    def weight(j, i):
        row = pl.ds(starts[j], min(chunk, ff - starts[j]))
        col = pl.ds(pl.multiple_of((t ^ order[i]) * block, 128), block)
        to = pl.ds(i * block, block)
        return [
            pltpu.make_async_copy(gate_h.at[row, col], gate_v.at[row, to], wsems.at[0, j, i]),
            pltpu.make_async_copy(up_h.at[row, col], up_v.at[row, to], wsems.at[1, j, i]),
        ]

    def down(i):
        col = pl.multiple_of((t ^ order[i]) * block, 128)
        return pltpu.make_async_copy(down_h.at[:, pl.ds(col, block)], down_v.at[i], dsems.at[i])

    def result(i):
        return pltpu.make_async_copy(out_v.at[i], outs[i], osems.at[i])

    for i in range(parts):
        for g in range(len(starts_x)):
            tokens(g, i).start()
        for copy in weight(0, i):
            copy.start()
    for j in range(1, len(starts)):
        for i in range(parts):
            for copy in weight(j, i):
                copy.start()
    for i in reversed(range(parts)):
        down(i).start()
    for g in range(len(starts_x)):
        for i in range(parts):
            tokens(g, i).wait()
    last = (((1,), (1,)), ((), ()))
    for j in range(len(starts)):
        for i in range(parts):
            for copy in weight(j, i):
                copy.wait()
        cut = slice(starts[j], min(starts[j] + chunk, ff))
        gate = lax.dot_general(x_v[...], gate_v[cut, :], last, preferred_element_type=F32)
        up = lax.dot_general(x_v[...], up_v[cut, :], last, preferred_element_type=F32)
        hid_v[:, cut] = (gate * jax.nn.sigmoid(gate) * up).astype(BF16)
    for i in reversed(range(parts)):
        down(i).wait()
        out_v[i] = jnp.dot(hid_v[...], down_v[i], preferred_element_type=F32).astype(BF16)
        result(i).start()
    for i in range(parts):
        result(i).wait()


def body(
    tokens_a,
    gain_a,
    value_w,
    gate_w,
    kernel,
    chan_gain,
    out_w,
    tokens_b,
    gain_b,
    routes,
    route_logits,
    expert_gate,
    expert_up,
    expert_down,
):
    experts = lax.axis_size("ep")
    bits = tp_bits()
    order = block_order(bits)
    parts = len(order)
    token_count, width = tokens_b.shape
    choices_per = routes.shape[1]
    capacity = 3 * token_count * choices_per // (2 * experts)
    block = width // parts
    slots = experts * capacity
    vmem = pl.BlockSpec(memory_space=pltpu.VMEM)
    anyw = pl.BlockSpec(memory_space=pl.ANY)

    comb_hi, comb_lo, *send = pl.pallas_call(
        functools.partial(prep_kernel, experts=experts, capacity=capacity, block=block),
        out_shape=(
            jax.ShapeDtypeStruct((slots, token_count), BF16),
            jax.ShapeDtypeStruct((slots, token_count), BF16),
        )
        + (jax.ShapeDtypeStruct((capacity, block), BF16),) * experts,
        in_specs=[vmem] * 4,
        out_specs=(vmem,) * (2 + experts),
        name="prep",
    )(tokens_b, gain_b[None, :], routes.T, route_logits.T)
    arrived = [swap(send[d], "ep", d) if d else send[d] for d in range(experts)]
    per = experts // 4
    inputs, starts_x = [], []
    for low, high in ((0, 2 * per), (2 * per, 3 * per), (3 * per, experts)):
        blocks = [jnp.concatenate(arrived[low:high], axis=0)]
        if not low:
            tokens_a, blocks[0] = lax.optimization_barrier((tokens_a, blocks[0]))
        for bit in reversed(bits):
            blocks = blocks + [swap(b, "tp", bit) for b in blocks]
        inputs += blocks
        starts_x.append(low * capacity)

    normed = rms_scaled(tokens_a, gain_a)
    contract_first = (((0,), (1,)), ((), ()))
    value_part = lax.dot_general(value_w, normed, contract_first, preferred_element_type=F32)
    gate_part = lax.dot_general(gate_w, normed, contract_first, preferred_element_type=F32)
    glu = (value_part * jax.nn.sigmoid(gate_part)).astype(BF16)
    taps = kernel.shape[0]
    length = glu.shape[1]
    rim = from_behind(glu[:, length - (taps - 1) :], "ep", 1)
    padded = jnp.concatenate([rim, glu], axis=1).astype(F32)
    mixed = jnp.zeros(glu.shape, F32)
    for tap in range(taps):
        mixed = mixed + kernel[tap][:, None] * padded[:, tap : tap + length]
    stats = jnp.stack([jnp.sum(mixed, axis=0), jnp.sum(mixed * mixed, axis=0)])
    for bit in bits:
        stats = stats + swap(stats, "tp", bit)
    channels = mixed.shape[0] * parts
    average = stats[0] / channels
    spread = stats[1] / channels - average * average
    normal_out = (
        (mixed - average[None, :]) * lax.rsqrt(spread + 1e-05)[None, :] * chan_gain[:, None]
    )
    activated = jax.nn.silu(normal_out).astype(BF16)
    conv = lax.dot_general(
        out_w, activated, (((0,), (0,)), ((), ())), preferred_element_type=F32
    ).astype(BF16)
    t = lax.axis_index("tp")
    picked = [lax.dynamic_slice_in_dim(conv, (t ^ o) * block, block, 0) for o in order]
    conv_out = jnp.concatenate(picked, axis=0)
    for bit in bits:
        rows = conv_out.shape[0] // 2
        got = swap(conv_out[rows:], "tp", bit)
        conv_out = (conv_out[:rows].astype(F32) + got.astype(F32)).astype(BF16)

    ff = expert_gate.shape[2]
    outs = pl.pallas_call(
        functools.partial(ffn_kernel, order=order, block=block, starts_x=starts_x),
        out_shape=(jax.ShapeDtypeStruct((slots, block), BF16),) * parts,
        in_specs=[anyw] * (len(inputs) + 3),
        out_specs=(anyw,) * parts,
        scratch_shapes=[
            pltpu.VMEM((slots, width), BF16),
            pltpu.VMEM((ff, width), BF16),
            pltpu.VMEM((ff, width), BF16),
            pltpu.VMEM((parts, ff, block), BF16),
            pltpu.VMEM((slots, ff), BF16),
            pltpu.VMEM((parts, slots, block), BF16),
            pltpu.SemaphoreType.DMA((len(starts_x), parts)),
            pltpu.SemaphoreType.DMA((2, -(-ff // 256), parts)),
            pltpu.SemaphoreType.DMA((parts,)),
            pltpu.SemaphoreType.DMA((parts,)),
        ],
        name="ffn",
        cost_estimate=pl.CostEstimate(
            flops=6 * slots * width * ff, bytes_accessed=6 * width * ff, transcendentals=slots * ff
        ),
    )(*inputs, expert_gate[0].T, expert_up[0].T, expert_down[0])
    sums = [[block_out] for block_out in outs]
    for bit in bits[:-1]:
        count = len(sums) // 2
        got = [None] * count
        for i in reversed(range(count)):
            terms = sums[count + i]
            whole = terms[0] if len(terms) == 1 else sum(x.astype(F32) for x in terms).astype(BF16)
            got[i] = swap(whole, "tp", bit)
        sums = [sums[i] + [got[i]] for i in range(count)]
    low_terms, high_terms = sums
    lows = []
    for d in range(experts):
        own = slice(d * capacity, (d + 1) * capacity)
        lows.append(sum(x[own].astype(F32) for x in low_terms).astype(BF16))
    lows = lax.optimization_barrier(tuple(lows))
    returned = [None] * experts
    for g in reversed(range(4)):
        rows = slice(g * per * capacity, (g + 1) * per * capacity)
        sent = sum(x[rows].astype(F32) for x in high_terms).astype(BF16)
        got = swap(sent, "tp", bits[-1])
        for i in range(per):
            d = g * per + i
            add = got[i * capacity : (i + 1) * capacity].astype(F32)
            piece = (lows[d].astype(F32) + add).astype(BF16)
            returned[d] = swap(piece, "ep", d) if d else piece
    rows = jnp.concatenate(returned, axis=0)
    last = (((0,), (0,)), ((), ()))
    moe_out = lax.dot_general(rows, comb_hi, last, preferred_element_type=F32)
    moe_out = moe_out + lax.dot_general(rows, comb_lo, last, preferred_element_type=F32)
    return (conv_out, moe_out.astype(BF16))


def solution(mesh):
    return jax.shard_map(
        body,
        mesh=mesh,
        in_specs=(
            P("ep", None),
            P(),
            P(None, "tp"),
            P(None, "tp"),
            P(None, "tp"),
            P("tp"),
            P("tp", None),
            P("ep", None),
            P(),
            P("ep", None),
            P("ep", None),
            P("ep", None, "tp"),
            P("ep", None, "tp"),
            P("ep", "tp", None),
        ),
        out_specs=(P("tp", "ep"), P("tp", "ep")),
        check_vma=False,
    )
```
